32 devices in a mesh: sp: 8 (over z, y), tp: 4 (over x, core).
Axes of the slice: x: 2, y: 2, z: 4, core: 2. Of those that a mesh axis runs over, the one named last changes fastest.
Arguments:
- inputs: bfloat16 [8192, 4, 2048], P('sp'), may hold values from -6 to 6
- norm_gain: float32 [2048], replicated, may hold values from 0.1 to 1.9
- pool_proj: bfloat16 [2048, 1024], P(None, 'tp'), may hold values from -0.125 to 0.125
- pool_gate_proj: bfloat16 [2048, 1024], P(None, 'tp'), may hold values from -0.125 to 0.125
- pool_mix: bfloat16 [8, 128, 128], P('tp'), may hold values from -0.5 to 0.5
- query_proj: bfloat16 [2048, 1024], P(None, 'tp'), may hold values from -0.125 to 0.125
- key_proj: bfloat16 [2048, 512], P(None, 'tp'), may hold values from -0.125 to 0.125
- value_proj: bfloat16 [2048, 512], P(None, 'tp'), may hold values from -0.125 to 0.125
- attn_gate_proj: bfloat16 [2048, 1024], P(None, 'tp'), may hold values from -0.125 to 0.125
- query_gain: float32 [64], replicated, may hold values from 0.1 to 1.9
- key_gain: float32 [64], replicated, may hold values from 0.1 to 1.9
- sink_logit: float32 [16], P('tp'), may hold values from -12 to 240
- out_pool: bfloat16 [1024, 2048], P('sp'), may hold values from -0.125 to 0.125
- out_attn: bfloat16 [1024, 2048], P('sp'), may hold values from -0.125 to 0.125
Outputs:
- mixed_out: bfloat16 [8192, 4, 2048], P(('sp', 'tp'))
- log_weight_sum: float32 [8192, 4, 16], P('sp', None, 'tp')
The draws below stay inside these ranges and needn't reach their ends.
All inputs are finite; a program needn't handle non-finite values.
Results may differ from the reference program's by a relative error of at most 0.015.
Values may be sent and summed in bfloat16 or wider, within the bound.
A program may use at most 192 MiB of HBM per device.

```python
import jax
import jax.numpy as jnp
from jax import lax

D = 2048
POOL_GROUPS = 8
GROUP_CH = 128
POOL_WIDTH = 1024
HEADS = 16
KV_HEADS = 8
HEAD_DIM = 64
GROUP_SIZE = 2
ATT_WIDTH = 1024
KV_WIDTH = 512
WINDOW = 128
SEQS = 4
SEQ_LEN = 8192


def draw_sink_logit(key, part):
    base = jnp.clip(2.0 * jax.random.normal(jax.random.fold_in(key, 1), (HEADS,), jnp.float32), -12.0, 12.0)
    return base


def shard_levels(stream_key, dims, shards, least, top_value):
    def one(dim, blocks):
        heights = jax.random.uniform(jax.random.fold_in(jax.random.fold_in(stream_key, 6), dim), (blocks,), jnp.float32, least / len(shards), top_value / len(shards))
        return jnp.repeat(jnp.exp(heights), dims[dim] // blocks).reshape((-1,) + (1,) * (len(dims) - dim - 1))

    factor_of = one(*shards[0])
    for cut in shards[1:]:
        factor_of = factor_of * one(*cut)
    return factor_of


def centred(stream_key, dims, width, reach, pieces=(), held_as=jnp.bfloat16):
    drawn = width * jax.random.normal(stream_key, dims, jnp.float32)
    if pieces:
        drawn = drawn * shard_levels(stream_key, dims, pieces, -0.22, 0.18)
    return jnp.clip(drawn, -reach, reach).astype(held_as)


def setup_inputs(seed: int = 0) -> dict:
    splits = jax.random.split(jax.random.key(seed), 15)
    inputs = centred(splits[0], (SEQ_LEN, SEQS, D), 1.0, 6.0, ((0, 8),))
    norm_gain = jnp.clip(1.0 + 0.18 * jax.random.normal(splits[1], (D,), jnp.float32), 0.1, 1.9)
    pool_proj = centred(splits[2], (D, POOL_WIDTH), D ** -0.5, 0.125, ((1, 4),))
    pool_gate_proj = centred(splits[3], (D, POOL_WIDTH), D ** -0.5, 0.125, ((1, 4),))
    pool_mix = centred(splits[4], (POOL_GROUPS, GROUP_CH, GROUP_CH), GROUP_CH ** -0.5, 0.5, ((0, 4),))
    query_proj = centred(splits[5], (D, ATT_WIDTH), D ** -0.5, 0.125, ((1, 4),))
    key_proj = centred(splits[6], (D, KV_WIDTH), D ** -0.5, 0.125, ((1, 4),))
    value_proj = centred(splits[7], (D, KV_WIDTH), D ** -0.5, 0.125, ((1, 4),))
    attn_gate_proj = centred(splits[8], (D, ATT_WIDTH), D ** -0.5, 0.125, ((1, 4),))
    query_gain = jnp.clip(1.0 + 0.18 * jax.random.normal(splits[9], (HEAD_DIM,), jnp.float32), 0.1, 1.9)
    key_gain = jnp.clip(1.0 + 0.18 * jax.random.normal(splits[10], (HEAD_DIM,), jnp.float32), 0.1, 1.9)
    sink_logit = draw_sink_logit(jax.random.fold_in(splits[14], 71), 0)
    out_pool = centred(splits[12], (POOL_WIDTH, D), (POOL_WIDTH + ATT_WIDTH) ** -0.5, 0.125, ((0, 8),))
    out_attn = centred(splits[13], (ATT_WIDTH, D), (POOL_WIDTH + ATT_WIDTH) ** -0.5, 0.125, ((0, 8),))
    return {"inputs": inputs, "norm_gain": norm_gain, "pool_proj": pool_proj, "pool_gate_proj": pool_gate_proj, "pool_mix": pool_mix, "query_proj": query_proj, "key_proj": key_proj, "value_proj": value_proj, "attn_gate_proj": attn_gate_proj, "query_gain": query_gain, "key_gain": key_gain, "sink_logit": sink_logit, "out_pool": out_pool, "out_attn": out_attn}


EPS = 1e-06
NEG = -1e+30

def stored(values):
    return lax.optimization_barrier(values.astype(jnp.bfloat16))

def reference(inputs, norm_gain, pool_proj, pool_gate_proj, pool_mix, query_proj, key_proj, value_proj, attn_gate_proj, query_gain, key_gain, sink_logit, out_pool, out_attn):
    seq_len = inputs.shape[0]
    flt = inputs.astype(jnp.float32)
    hidden = stored(flt * lax.rsqrt(lax.optimization_barrier(jnp.mean(flt * flt, axis=-1, keepdims=True)) + EPS) * norm_gain.astype(jnp.float32))

    def project(weight):
        return stored(jnp.dot(hidden, weight, preferred_element_type=jnp.float32))
    pool_in = project(pool_proj)
    pool_gate = project(pool_gate_proj)
    queries = project(query_proj)
    key_rows = project(key_proj)
    value_rows = project(value_proj)
    attn_gate = project(attn_gate_proj)
    pool_f = pool_in.astype(jnp.float32).reshape(seq_len, SEQS, POOL_GROUPS, GROUP_CH)
    prefix = jnp.concatenate([jnp.zeros((1, SEQS, POOL_GROUPS, GROUP_CH), jnp.float32), jnp.cumsum(pool_f, axis=0)], axis=0)
    positions = jnp.arange(seq_len, dtype=jnp.int32)
    means = []
    for group_id in range(POOL_GROUPS):
        half_width = 2 ** (group_id % 4)
        low_pos = jnp.clip(positions - half_width, 0, seq_len - 1)
        high_pos = jnp.clip(positions + half_width - 1, 0, seq_len - 1)
        window_sum = prefix[high_pos + 1, :, group_id] - prefix[low_pos, :, group_id]
        count_live = (high_pos - low_pos + 1).astype(jnp.float32)[:, None, None]
        means.append(window_sum / count_live)
    pooled = stored(jnp.stack(means, axis=2) - pool_f)
    pool_mixed = jnp.einsum('lsgc,gcd->lsgd', pooled.astype(jnp.float32), pool_mix.astype(jnp.float32))
    pool_mixed = pool_mixed.reshape(seq_len, SEQS, POOL_WIDTH)
    y_pool = stored(pool_mixed * jax.nn.silu(pool_gate.astype(jnp.float32)))

    def head_norm(values, heads, gain):
        flt_heads = values.astype(jnp.float32).reshape(seq_len, SEQS, heads, HEAD_DIM)
        return stored(flt_heads * lax.rsqrt(lax.optimization_barrier(jnp.mean(flt_heads * flt_heads, axis=-1, keepdims=True)) + EPS) * gain.astype(jnp.float32))
    normed_q = head_norm(queries, HEADS, query_gain).reshape(seq_len, SEQS, KV_HEADS, GROUP_SIZE, HEAD_DIM)
    normed_k = head_norm(key_rows, KV_HEADS, key_gain)
    value_heads = value_rows.reshape(seq_len, SEQS, KV_HEADS, HEAD_DIM)
    padding = ((WINDOW, WINDOW), (0, 0), (0, 0), (0, 0))
    key_pad = jnp.pad(normed_k, padding)
    value_pad = jnp.pad(value_heads, padding)
    slopes = (2.0 ** (-8.0 * jnp.arange(1, HEADS + 1, dtype=jnp.float32) / HEADS)).reshape(KV_HEADS, GROUP_SIZE)
    sink_vals = sink_logit.astype(jnp.float32).reshape(KV_HEADS, GROUP_SIZE)[None, :, :, None]

    def block(index):
        query_block = lax.dynamic_slice_in_dim(normed_q, index * WINDOW, WINDOW, 0)
        key_block = lax.dynamic_slice_in_dim(key_pad, index * WINDOW, 3 * WINDOW, 0)
        value_block = lax.dynamic_slice_in_dim(value_pad, index * WINDOW, 3 * WINDOW, 0)
        scores = jnp.einsum('qskgd,jskd->skgqj', query_block.astype(jnp.float32), key_block.astype(jnp.float32)) * HEAD_DIM ** (-0.5)
        query_pos = index * WINDOW + jnp.arange(WINDOW, dtype=jnp.int32)
        key_pos = index * WINDOW - WINDOW + jnp.arange(3 * WINDOW, dtype=jnp.int32)
        distance = jnp.abs(query_pos[:, None] - key_pos[None, :])
        usable = (distance <= WINDOW) & (key_pos >= 0)[None, :] & (key_pos < seq_len)[None, :]
        scores = scores - slopes[None, :, :, None, None] * distance.astype(jnp.float32)
        scores = jnp.where(usable, scores, NEG)
        row_top = jnp.maximum(lax.optimization_barrier(jnp.max(scores, axis=-1)), sink_vals)
        weights = jnp.exp(scores - row_top[..., None])
        weight_total = lax.optimization_barrier(jnp.sum(weights, axis=-1)) + jnp.exp(sink_vals - row_top)
        log_sum = row_top + jnp.log(weight_total)
        attended = jnp.einsum('skgqj,jskd->qskgd', stored(weights).astype(jnp.float32), value_block.astype(jnp.float32))
        attended = attended / jnp.transpose(weight_total, (3, 0, 1, 2))[..., None]
        return (attended.reshape(WINDOW, SEQS, ATT_WIDTH), jnp.transpose(log_sum, (3, 0, 1, 2)).reshape(WINDOW, SEQS, HEADS))
    attended, log_sums = lax.map(block, jnp.arange(seq_len // WINDOW, dtype=jnp.int32))
    attended = attended.reshape(seq_len, SEQS, ATT_WIDTH)
    log_weight_sum = log_sums.reshape(seq_len, SEQS, HEADS)
    y_attn = stored(attended * jax.nn.silu(attn_gate.astype(jnp.float32)))
    summed = jnp.dot(y_pool, out_pool, preferred_element_type=jnp.float32) + jnp.dot(y_attn, out_attn, preferred_element_type=jnp.float32)
    return (summed.astype(jnp.bfloat16), log_weight_sum)
```

```python
import functools
import math

import jax
import jax.numpy as jnp
from jax import lax
from jax.experimental import pallas as pl
from jax.experimental.pallas import tpu as pltpu
from jax.sharding import PartitionSpec as P

HEADS = 16
HEAD_DIM = 64
WINDOW = 128
EPS = 1e-06
NEG = -1e30
LOG2E = math.log2(math.e)
REACH = 16
BLK = 128
F32 = jnp.float32
BF16 = jnp.bfloat16


def halo(shard, width):
    count, length = lax.axis_size("sp"), shard.shape[1]
    up = [(i, i + 1) for i in range(count - 1)]
    down = [(j, i) for i, j in up]
    before = lax.ppermute(shard[:, length - width :], "sp", up)
    after = lax.ppermute(shard[:, :width], "sp", down)
    return before, after


def head_ones(cols):
    a = lax.broadcasted_iota(jnp.int32, (cols, cols), 0) // HEAD_DIM
    b = lax.broadcasted_iota(jnp.int32, (cols, cols), 1) // HEAD_DIM
    return jnp.where(a == b, 1.0 / HEAD_DIM, 0.0).astype(BF16)


def head_norm(values, gain):
    flt = values.astype(F32)
    mean = jnp.dot((flt * flt).astype(BF16), head_ones(flt.shape[-1]), preferred_element_type=F32)
    return (flt * lax.rsqrt(mean + EPS) * gain).astype(BF16)


def silu(gate):
    flt = gate.astype(F32)
    return flt / (1.0 + jnp.exp(-flt))


def mix_kernel(
    pc, qc, kc, total_len,
    ints, floats, proj, kv_before, kv_after, pool_before, pool_after, mix, q_gain, k_gain,
    y_pool, y_attn, lse,
    keys, vals, pool_pad, bias, band,
):
    length = proj.shape[1]
    rows = y_pool.shape[2]
    n_kv = kc // HEAD_DIM
    n_q = qc // HEAD_DIM
    groups = mix.shape[0]
    chan = mix.shape[1]
    offset = ints[0]
    c_gate, c_q, c_ag, c_kv = pc, 2 * pc, 2 * pc + qc, 2 * pc + 2 * qc
    half_pad = 64

    @pl.when(pl.program_id(0) == 0)
    def _():
        i = lax.broadcasted_iota(jnp.int32, (BLK, 3 * WINDOW), 0)
        j = lax.broadcasted_iota(jnp.int32, (BLK, 3 * WINDOW), 1) - WINDOW
        dist = jnp.abs(i - j)
        for h in range(n_q):
            value = -floats[0, h] * dist.astype(F32) - floats[1, h]
            bias[h] = jnp.where(dist <= WINDOW, value, NEG)
        ti = lax.broadcasted_iota(jnp.int32, (BLK, 2 * BLK), 0)
        tj = lax.broadcasted_iota(jnp.int32, (BLK, 2 * BLK), 1) - half_pad
        rel = tj - ti
        for g in range(groups):
            hw = ints[1 + g]
            inside = (rel >= -hw) & (rel <= hw - 1)
            band[g] = jnp.where(inside, 1.0, 0.0).astype(BF16)
        edge = jnp.zeros((half_pad - REACH, pc), BF16)
        pool_pad[0 : half_pad - REACH] = edge
        pool_pad[half_pad + length + REACH :] = edge

    pool_pad[half_pad - REACH : half_pad] = pool_before[0]
    pool_pad[half_pad : half_pad + length] = proj[0, :, :pc]
    pool_pad[half_pad + length : half_pad + length + REACH] = pool_after[0]

    def fill(first, count, kv):
        normed = head_norm(kv[:, :kc], k_gain[...])
        pos = lax.broadcasted_iota(jnp.int32, (count, HEAD_DIM), 0) + (offset + first - WINDOW)
        ones = jnp.where((pos >= 0) & (pos < total_len), 1.0, 0.0).astype(BF16)
        for p in range(n_kv):
            k = normed[:, p * HEAD_DIM : (p + 1) * HEAD_DIM]
            v = kv[:, kc + p * HEAD_DIM : kc + (p + 1) * HEAD_DIM]
            keys[p, first : first + count] = jnp.concatenate([k, k], axis=1)
            vals[2 * p, first : first + count] = jnp.concatenate([v, ones], axis=1)
            vals[2 * p + 1, first : first + count] = jnp.concatenate([ones, v], axis=1)

    fill(0, WINDOW, kv_before[0])
    fill(WINDOW, length, proj[0, :, c_kv:])
    fill(WINDOW + length, WINDOW, kv_after[0])

    low = lax.broadcasted_iota(jnp.int32, (BLK, 2 * HEAD_DIM), 1) < HEAD_DIM

    def step(b, carry):
        start = pl.multiple_of(b * BLK, BLK)
        dest = start // rows
        row = pl.multiple_of(start % rows, BLK)
        here = pl.ds(start, BLK)
        gpos = offset + start + lax.broadcasted_iota(jnp.int32, (BLK, chan), 0)
        for g in range(groups):
            hw = ints[1 + g]
            cols = slice(g * chan, (g + 1) * chan)
            window = jnp.dot(band[g], pool_pad[pl.ds(start, 2 * BLK), cols], preferred_element_type=F32)
            lo = jnp.maximum(gpos - hw, 0)
            hi = jnp.minimum(gpos + hw - 1, total_len - 1)
            live = (hi - lo + 1).astype(F32)
            pooled = (window / live - proj[0, here, cols].astype(F32)).astype(BF16)
            mixed = jnp.dot(pooled, mix[g], preferred_element_type=F32)
            gate = proj[0, here, c_gate + g * chan : c_gate + (g + 1) * chan]
            y_pool[dest, 0, pl.ds(row, BLK), cols] = (mixed * silu(gate)).astype(BF16)
        queries = head_norm(proj[0, here, c_q : c_q + qc], q_gain[...])
        for p in range(n_kv):
            pair = queries[:, p * 128 : (p + 1) * 128]
            zero = jnp.zeros_like(pair)
            stacked = jnp.concatenate([jnp.where(low, pair, zero), jnp.where(low, zero, pair)], axis=0)
            span = pl.ds(start, 3 * WINDOW)
            scores = lax.dot_general(
                stacked, keys[p, span], (((1,), (1,)), ((), ())), preferred_element_type=F32
            )
            w0 = jnp.exp2(scores[:BLK] + bias[2 * p]).astype(BF16)
            w1 = jnp.exp2(scores[BLK:] + bias[2 * p + 1]).astype(BF16)
            o0 = jnp.dot(w0, vals[2 * p, span], preferred_element_type=F32)
            o1 = jnp.dot(w1, vals[2 * p + 1, span], preferred_element_type=F32)
            num = jnp.where(low, o0, o1)
            tot = jnp.where(low, o1, o0) + 1.0
            den = pltpu.roll(tot, HEAD_DIM, 1)
            gate = proj[0, here, c_ag + p * 128 : c_ag + (p + 1) * 128]
            y_attn[dest, 0, pl.ds(row, BLK), p * 128 : (p + 1) * 128] = (num / den * silu(gate)).astype(BF16)
            tt = jnp.transpose(tot)
            lse[0, 2 * p : 2 * p + 1, here] = floats[2, 2 * p] + jnp.log(tt[HEAD_DIM : HEAD_DIM + 1])
            lse[0, 2 * p + 1 : 2 * p + 2, here] = floats[2, 2 * p + 1] + jnp.log(tt[0:1])
        return carry

    lax.fori_loop(0, length // BLK, step, 0)


def out_kernel(tp, pool_rows, attn_rows, w_pool, w_attn, out):
    width = pool_rows.shape[-1]
    acc = None
    for rows_ref, w_ref in ((pool_rows, w_pool), (attn_rows, w_attn)):
        lhs = jnp.concatenate([rows_ref[p, 0] for p in range(tp)], axis=1)
        part = jnp.dot(lhs, w_ref[...], preferred_element_type=F32)
        acc = part if acc is None else acc + part
    out[0] = acc.astype(BF16)


def body(
    inputs, norm_gain, pool_proj, pool_gate_proj, pool_mix, query_proj, key_proj, value_proj,
    attn_gate_proj, query_gain, key_gain, sink_logit, out_pool, out_attn,
):
    length, seqs, model = inputs.shape
    tp = lax.axis_size("tp")
    tp_index = lax.axis_index("tp")
    offset = lax.axis_index("sp") * length
    total_len = length * lax.axis_size("sp")
    pc, qc, kc = pool_proj.shape[1], query_proj.shape[1], key_proj.shape[1]
    width = 2 * pc + 2 * qc + 2 * kc
    n_q = qc // HEAD_DIM
    n_kv = kc // HEAD_DIM
    groups = pool_mix.shape[0]
    rows = length // tp

    w_pool = lax.all_gather(out_pool, "sp", axis=0, tiled=True)
    w_attn = lax.all_gather(out_attn, "sp", axis=0, tiled=True)

    flt = inputs.astype(F32)
    scale = lax.rsqrt(jnp.mean(flt * flt, axis=-1) + EPS)
    weights = jnp.concatenate(
        [pool_proj, pool_gate_proj, query_proj, attn_gate_proj, key_proj, value_proj], axis=1
    )
    weights = (weights.astype(F32) * norm_gain[:, None]).astype(BF16)
    proj = jnp.einsum("tsd,dc->stc", inputs, weights, preferred_element_type=F32)
    proj = (proj * scale.T[:, :, None]).astype(BF16)

    kv_before, kv_after = halo(proj[:, :, 2 * pc + 2 * qc :], WINDOW)
    pool_before, pool_after = halo(proj[:, :, :pc], REACH)

    head_ids = tp_index * n_q + jnp.arange(n_q, dtype=jnp.int32)
    slopes = 2.0 ** (-8.0 * (head_ids + 1).astype(F32) / HEADS)
    floats = jnp.stack([slopes * LOG2E, sink_logit * LOG2E, sink_logit])
    half_widths = jnp.left_shift(
        jnp.int32(1), (tp_index * groups + jnp.arange(groups, dtype=jnp.int32)) % 4
    )
    ints = jnp.concatenate([offset[None].astype(jnp.int32), half_widths])
    q_gain = jnp.tile(query_gain * (HEAD_DIM**-0.5 * LOG2E), n_q)[None]
    k_gain = jnp.tile(key_gain, n_kv)[None]

    smem = pl.BlockSpec(memory_space=pltpu.SMEM)
    full = lambda shape: pl.BlockSpec(shape, lambda s: (0,) * len(shape))
    per_seq = lambda *shape: pl.BlockSpec((1,) + shape, lambda s: (s,) + (0,) * len(shape))
    y_pool, y_attn, lse = pl.pallas_call(
        functools.partial(mix_kernel, pc, qc, kc, total_len),
        grid=(seqs,),
        in_specs=[
            smem, smem,
            per_seq(length, width),
            per_seq(WINDOW, 2 * kc), per_seq(WINDOW, 2 * kc),
            per_seq(REACH, pc), per_seq(REACH, pc),
            full(pool_mix.shape), full((1, qc)), full((1, kc)),
        ],
        out_specs=[
            pl.BlockSpec((tp, 1, rows, pc), lambda s: (0, s, 0, 0)),
            pl.BlockSpec((tp, 1, rows, qc), lambda s: (0, s, 0, 0)),
            per_seq(n_q, length),
        ],
        out_shape=[
            jax.ShapeDtypeStruct((tp, seqs, rows, pc), BF16),
            jax.ShapeDtypeStruct((tp, seqs, rows, qc), BF16),
            jax.ShapeDtypeStruct((seqs, n_q, length), F32),
        ],
        scratch_shapes=[
            pltpu.VMEM((n_kv, length + 2 * WINDOW, 128), BF16),
            pltpu.VMEM((n_q, length + 2 * WINDOW, 128), BF16),
            pltpu.VMEM((length + 128, pc), BF16),
            pltpu.VMEM((n_q, BLK, 3 * WINDOW), F32),
            pltpu.VMEM((groups, BLK, 2 * BLK), BF16),
        ],
        name="mixers",
    )(ints, floats, proj, kv_before, kv_after, pool_before, pool_after, pool_mix, q_gain, k_gain)

    pool_rows = lax.all_to_all(y_pool, "tp", split_axis=0, concat_axis=0, tiled=True)
    attn_rows = lax.all_to_all(y_attn, "tp", split_axis=0, concat_axis=0, tiled=True)

    mixed = pl.pallas_call(
        functools.partial(out_kernel, tp),
        grid=(seqs,),
        in_specs=[
            pl.BlockSpec((tp, 1, rows, pc), lambda s: (0, s, 0, 0)),
            pl.BlockSpec((tp, 1, rows, qc), lambda s: (0, s, 0, 0)),
            full(w_pool.shape), full(w_attn.shape),
        ],
        out_specs=per_seq(rows, model),
        out_shape=jax.ShapeDtypeStruct((seqs, rows, model), BF16),
        name="outproj",
    )(pool_rows, attn_rows, w_pool, w_attn)
    return jnp.transpose(mixed, (1, 0, 2)), jnp.transpose(lse, (2, 0, 1))


def solution(mesh):
    placed = (
        P("sp", None, None), P(), P(None, "tp"), P(None, "tp"), P("tp", None, None),
        P(None, "tp"), P(None, "tp"), P(None, "tp"), P(None, "tp"),
        P(), P(), P("tp"), P("sp", None), P("sp", None),
    )
    return jax.shard_map(
        body,
        mesh=mesh,
        in_specs=placed,
        out_specs=(P(("sp", "tp"), None, None), P("sp", None, "tp")),
        check_vma=False,
    )
```

```python
import functools
import math

import jax
import jax.numpy as jnp
from jax import lax
from jax.experimental import pallas as pl
from jax.experimental.pallas import tpu as pltpu
from jax.sharding import PartitionSpec as P

HEADS = 16
HEAD_DIM = 64
WINDOW = 128
EPS = 1e-06
NEG = -1e30
LOG2E = math.log2(math.e)
REACH = 16
BLK = 128
F32 = jnp.float32
BF16 = jnp.bfloat16
MESH = pl.DeviceIdType.MESH


def head_ones(cols):
    a = lax.broadcasted_iota(jnp.int32, (cols, cols), 0) // HEAD_DIM
    b = lax.broadcasted_iota(jnp.int32, (cols, cols), 1) // HEAD_DIM
    return jnp.where(a == b, 1.0 / HEAD_DIM, 0.0).astype(BF16)


def head_norm(values, gain):
    flt = values.astype(F32)
    mean = jnp.dot((flt * flt).astype(BF16), head_ones(flt.shape[-1]), preferred_element_type=F32)
    return (flt * lax.rsqrt(mean + EPS) * gain).astype(BF16)


def silu(gate):
    flt = gate.astype(F32)
    return flt / (1.0 + jnp.exp(-flt))


def mix_kernel(
    pc, qc, kc, count, tp, seqs, length, total_len,
    floats, proj, proj_any, w_any, mix, q_gain, k_gain,
    out, lse,
    keys, vals, pool_pad, bias, band, kv_halo, pool_halo, y_buf, y_recv, w_buf,
    halo_send, halo_recv, y_send, y_got, y_local, w_sems,
):
    rows = length // tp
    n_kv = kc // HEAD_DIM
    n_q = qc // HEAD_DIM
    groups = mix.shape[0]
    chan = mix.shape[1]
    i = pl.program_id(0)
    sp_me, me = lax.axis_index("sp"), lax.axis_index("tp")
    offset = sp_me * length
    half_widths = [jnp.left_shift(jnp.int32(1), (me * groups + g) % 4) for g in range(groups)]
    c_gate, c_q, c_ag, c_kv = pc, 2 * pc, 2 * pc + qc, 2 * pc + 2 * qc
    half_pad = 64
    core = me % 2
    sibling = me + 1 - 2 * core
    after = (sp_me + 1) % count
    before = (sp_me + count - 1) % count
    peers = [(me + d) % tp for d in range(1, tp)]

    def halo_copies(s):
        made = []
        for side, (target, first) in enumerate(((after, True), (before, False))):
            for kind, (buf, width, col, cols) in enumerate(
                ((kv_halo, WINDOW, c_kv, 2 * kc), (pool_halo, REACH, 0, pc))
            ):
                start = length - width if first else 0
                made.append(
                    pltpu.make_async_remote_copy(
                        src_ref=proj_any.at[s, pl.ds(start, width), pl.ds(col, cols)],
                        dst_ref=buf.at[side, s],
                        send_sem=halo_send.at[side, kind, s],
                        recv_sem=halo_recv.at[side, kind, s],
                        device_id={"sp": target},
                        device_id_type=MESH,
                    )
                )
        return made

    def y_copies(s):
        return [
            pltpu.make_async_remote_copy(
                src_ref=y_buf.at[s, peer],
                dst_ref=y_recv.at[me, s],
                send_sem=y_send.at[d, s],
                recv_sem=y_got.at[d, s],
                device_id={"tp": peer},
                device_id_type=MESH,
            )
            for d, peer in enumerate(peers)
        ]

    def y_own(s):
        return pltpu.make_async_copy(y_buf.at[s, me], y_recv.at[me, s], y_local.at[s])

    def w_copies():
        return (
            pltpu.make_async_remote_copy(
                src_ref=w_any, dst_ref=w_buf.at[core], send_sem=w_sems.at[0], recv_sem=w_sems.at[1],
                device_id={"tp": sibling}, device_id_type=MESH,
            ),
            pltpu.make_async_copy(w_any, w_buf.at[core], w_sems.at[2]),
        )

    @pl.when(i == 0)
    def _():
        barrier = pltpu.get_barrier_semaphore()
        for target in (after, before):
            pl.semaphore_signal(barrier, inc=1, device_id={"sp": target}, device_id_type=MESH)
        for peer in peers:
            pl.semaphore_signal(barrier, inc=1, device_id={"tp": peer}, device_id_type=MESH)
        pl.semaphore_wait(barrier, 2 + len(peers))
        for s in range(seqs):
            for copy in halo_copies(s):
                copy.start()
        for copy in w_copies():
            copy.start()
        ii = lax.broadcasted_iota(jnp.int32, (BLK, 3 * WINDOW), 0)
        jj = lax.broadcasted_iota(jnp.int32, (BLK, 3 * WINDOW), 1) - WINDOW
        dist = jnp.abs(ii - jj)
        for h in range(n_q):
            value = -floats[0, h] * dist.astype(F32) - floats[1, h]
            bias[h] = jnp.where(dist <= WINDOW, value, NEG)
        ti = lax.broadcasted_iota(jnp.int32, (BLK, 2 * BLK), 0)
        tj = lax.broadcasted_iota(jnp.int32, (BLK, 2 * BLK), 1) - half_pad
        rel = tj - ti
        for g in range(groups):
            hw = half_widths[g]
            inside = (rel >= -hw) & (rel <= hw - 1)
            band[g] = jnp.where(inside, 1.0, 0.0).astype(BF16)
        edge = jnp.zeros((half_pad - REACH, pc), BF16)
        pool_pad[0 : half_pad - REACH] = edge
        pool_pad[half_pad + length + REACH :] = edge

    def fill(first, size, kv):
        normed = head_norm(kv[:, :kc], k_gain[...])
        pos = lax.broadcasted_iota(jnp.int32, (size, HEAD_DIM), 0) + (offset + first - WINDOW)
        valid = (pos >= 0) & (pos < total_len)
        ones = jnp.where(valid, 1.0, 0.0).astype(BF16)
        for p in range(n_kv):
            k = normed[:, p * HEAD_DIM : (p + 1) * HEAD_DIM]
            v = kv[:, kc + p * HEAD_DIM : kc + (p + 1) * HEAD_DIM] * ones
            keys[p, first : first + size] = jnp.concatenate([k, k], axis=1)
            vals[2 * p, first : first + size] = jnp.concatenate([v, ones], axis=1)
            vals[2 * p + 1, first : first + size] = jnp.concatenate([ones, v], axis=1)

    low = lax.broadcasted_iota(jnp.int32, (BLK, 2 * HEAD_DIM), 1) < HEAD_DIM

    def step(b, carry):
        start = pl.multiple_of(b * BLK, BLK)
        dest = start // rows
        row = pl.multiple_of(start % rows, BLK)
        here = pl.ds(start, BLK)
        gpos = offset + start + lax.broadcasted_iota(jnp.int32, (BLK, chan), 0)
        for g in range(groups):
            hw = half_widths[g]
            cols = slice(g * chan, (g + 1) * chan)
            window = jnp.dot(band[g], pool_pad[pl.ds(start, 2 * BLK), cols], preferred_element_type=F32)
            lo = jnp.maximum(gpos - hw, 0)
            hi = jnp.minimum(gpos + hw - 1, total_len - 1)
            live = (hi - lo + 1).astype(F32)
            pooled = (window / live - proj[0, here, cols].astype(F32)).astype(BF16)
            mixed = jnp.dot(pooled, mix[g], preferred_element_type=F32)
            gate = proj[0, here, c_gate + g * chan : c_gate + (g + 1) * chan]
            y_buf[i, dest, pl.ds(row, BLK), cols] = (mixed * silu(gate)).astype(BF16)
        queries = head_norm(proj[0, here, c_q : c_q + qc], q_gain[...])
        for p in range(n_kv):
            pair = queries[:, p * 128 : (p + 1) * 128]
            zero = jnp.zeros_like(pair)
            stacked = jnp.concatenate([jnp.where(low, pair, zero), jnp.where(low, zero, pair)], axis=0)
            span = pl.ds(start, 3 * WINDOW)
            scores = lax.dot_general(
                stacked, keys[p, span], (((1,), (1,)), ((), ())), preferred_element_type=F32
            )
            w0 = jnp.exp2(scores[:BLK] + bias[2 * p]).astype(BF16)
            w1 = jnp.exp2(scores[BLK:] + bias[2 * p + 1]).astype(BF16)
            o0 = jnp.dot(w0, vals[2 * p, span], preferred_element_type=F32)
            o1 = jnp.dot(w1, vals[2 * p + 1, span], preferred_element_type=F32)
            num = jnp.where(low, o0, o1)
            tot = jnp.where(low, o1, o0) + 1.0
            den = pltpu.roll(tot, HEAD_DIM, 1)
            gate = proj[0, here, c_ag + p * 128 : c_ag + (p + 1) * 128]
            y_buf[i, dest, pl.ds(row, BLK), pc + p * 128 : pc + (p + 1) * 128] = (
                num / den * silu(gate)
            ).astype(BF16)
            tt = jnp.transpose(tot)
            lse[0, 2 * p : 2 * p + 1, here] = floats[2, 2 * p] + jnp.log(tt[HEAD_DIM : HEAD_DIM + 1])
            lse[0, 2 * p + 1 : 2 * p + 2, here] = floats[2, 2 * p + 1] + jnp.log(tt[0:1])
        return carry

    @pl.when(i < seqs)
    def _():
        pool_pad[half_pad : half_pad + length] = proj[0, :, :pc]
        fill(WINDOW, length, proj[0, :, c_kv:])
        for copy in halo_copies(i):
            copy.wait()
        first = jnp.where(sp_me > 0, 1.0, 0.0).astype(BF16)
        last = jnp.where(sp_me < count - 1, 1.0, 0.0).astype(BF16)
        pool_pad[half_pad - REACH : half_pad] = pool_halo[0, i] * first
        pool_pad[half_pad + length : half_pad + length + REACH] = pool_halo[1, i] * last
        fill(0, WINDOW, kv_halo[0, i])
        fill(WINDOW + length, WINDOW, kv_halo[1, i])
        lax.fori_loop(0, length // BLK, step, 0)
        for copy in y_copies(i):
            copy.start()
        y_own(i).start()

    @pl.when(i == seqs)
    def _():
        for copy in w_copies():
            copy.wait()

    @pl.when(i >= seqs)
    def _():
        s = i - seqs
        for copy in y_copies(s):
            copy.wait()
        y_own(s).wait()
        half = out.shape[-1] // 2
        depth = w_buf.shape[1] * w_buf.shape[3]
        pool_rows = jnp.concatenate([y_recv[p, s, :, :pc] for p in range(tp)], axis=1)
        attn_rows = jnp.concatenate([y_recv[p, s, :, pc:] for p in range(tp)], axis=1)
        for h in range(2):
            acc = jnp.dot(pool_rows, w_buf[h, :, 0].reshape(depth, half), preferred_element_type=F32)
            acc = acc + jnp.dot(attn_rows, w_buf[h, :, 1].reshape(depth, half), preferred_element_type=F32)
            out[0, :, h * half : (h + 1) * half] = acc.astype(BF16)


def body(
    inputs, norm_gain, pool_proj, pool_gate_proj, pool_mix, query_proj, key_proj, value_proj,
    attn_gate_proj, query_gain, key_gain, sink_logit, out_pool, out_attn,
):
    length, seqs, model = inputs.shape
    tp = lax.axis_size("tp")
    tp_index = lax.axis_index("tp")
    count = lax.axis_size("sp")
    total_len = length * count
    pc, qc, kc = pool_proj.shape[1], query_proj.shape[1], key_proj.shape[1]
    width = 2 * pc + 2 * qc + 2 * kc
    n_q = qc // HEAD_DIM
    n_kv = kc // HEAD_DIM
    groups = pool_mix.shape[0]
    rows = length // tp

    half = model // 2
    w_half = jnp.stack([out_pool, out_attn])
    w_half = lax.dynamic_slice_in_dim(w_half, (tp_index % 2) * half, half, 2)
    w_half = lax.all_gather(w_half, "sp", axis=0)

    flt = inputs.astype(F32)
    scale = lax.rsqrt(jnp.mean(flt * flt, axis=-1) + EPS)
    weights = jnp.concatenate(
        [pool_proj, pool_gate_proj, query_proj, attn_gate_proj, key_proj, value_proj], axis=1
    )
    weights = (weights.astype(F32) * norm_gain[:, None]).astype(BF16)
    proj = jnp.einsum("tsd,dc->stc", inputs, weights, preferred_element_type=F32)
    proj = (proj * scale.T[:, :, None]).astype(BF16)

    head_ids = tp_index * n_q + jnp.arange(n_q, dtype=jnp.int32)
    slopes = 2.0 ** (-8.0 * (head_ids + 1).astype(F32) / HEADS)
    floats = jnp.stack([slopes * LOG2E, sink_logit * LOG2E, sink_logit])
    q_gain = jnp.tile(query_gain * (HEAD_DIM**-0.5 * LOG2E), n_q)[None]
    k_gain = jnp.tile(key_gain, n_kv)[None]

    smem = pl.BlockSpec(memory_space=pltpu.SMEM)
    full = lambda shape: pl.BlockSpec(shape, lambda s: (0,) * len(shape))
    anywhere = pl.BlockSpec(memory_space=pl.ANY)
    early = lambda *shape: pl.BlockSpec(
        (1,) + shape, lambda i: (jnp.minimum(i, seqs - 1),) + (0,) * len(shape)
    )
    late = lambda *shape: pl.BlockSpec(
        (1,) + shape, lambda i: (jnp.maximum(i - seqs, 0),) + (0,) * len(shape)
    )
    dma = lambda *shape: pltpu.SemaphoreType.DMA(shape)
    mixed, lse = pl.pallas_call(
        functools.partial(mix_kernel, pc, qc, kc, count, tp, seqs, length, total_len),
        grid=(2 * seqs,),
        in_specs=[
            smem, early(length, width), anywhere, anywhere,
            full(pool_mix.shape), full((1, qc)), full((1, kc)),
        ],
        out_specs=[late(rows, model), early(n_q, length)],
        out_shape=[
            jax.ShapeDtypeStruct((seqs, rows, model), BF16),
            jax.ShapeDtypeStruct((seqs, n_q, length), F32),
        ],
        scratch_shapes=[
            pltpu.VMEM((n_kv, length + 2 * WINDOW, 128), BF16),
            pltpu.VMEM((n_q, length + 2 * WINDOW, 128), BF16),
            pltpu.VMEM((length + 128, pc), BF16),
            pltpu.VMEM((n_q, BLK, 3 * WINDOW), F32),
            pltpu.VMEM((groups, BLK, 2 * BLK), BF16),
            pltpu.VMEM((2, seqs, WINDOW, 2 * kc), BF16),
            pltpu.VMEM((2, seqs, REACH, pc), BF16),
            pltpu.VMEM((seqs, tp, rows, pc + qc), BF16),
            pltpu.VMEM((tp, seqs, rows, pc + qc), BF16),
            pltpu.VMEM((2,) + w_half.shape, BF16),
            dma(2, 2, seqs), dma(2, 2, seqs),
            dma(tp - 1, seqs), dma(tp - 1, seqs), dma(seqs), dma(3),
        ],
        compiler_params=pltpu.CompilerParams(collective_id=0, has_side_effects=True),
        name="mixers",
    )(floats, proj, proj, w_half, pool_mix, q_gain, k_gain)
    return jnp.transpose(mixed, (1, 0, 2)), jnp.transpose(lse, (2, 0, 1))


def solution(mesh):
    placed = (
        P("sp", None, None), P(), P(None, "tp"), P(None, "tp"), P("tp", None, None),
        P(None, "tp"), P(None, "tp"), P(None, "tp"), P(None, "tp"),
        P(), P(), P("tp"), P("sp", None), P("sp", None),
    )
    return jax.shard_map(
        body,
        mesh=mesh,
        in_specs=placed,
        out_specs=(P(("sp", "tp"), None, None), P("sp", None, "tp")),
        check_vma=False,
    )
```

```python
import functools
import math

import jax
import jax.numpy as jnp
from jax import lax
from jax.experimental import pallas as pl
from jax.experimental.pallas import tpu as pltpu
from jax.sharding import PartitionSpec as P

HEADS = 16
HEAD_DIM = 64
WINDOW = 128
EPS = 1e-06
NEG = -1e30
LOG2E = math.log2(math.e)
REACH = 16
BLK = 128
F32 = jnp.float32
BF16 = jnp.bfloat16
MESH = pl.DeviceIdType.MESH


def head_ones(cols):
    a = lax.broadcasted_iota(jnp.int32, (cols, cols), 0) // HEAD_DIM
    b = lax.broadcasted_iota(jnp.int32, (cols, cols), 1) // HEAD_DIM
    return jnp.where(a == b, 1.0 / HEAD_DIM, 0.0).astype(BF16)


def head_norm(values, gain):
    flt = values.astype(F32)
    mean = jnp.dot((flt * flt).astype(BF16), head_ones(flt.shape[-1]), preferred_element_type=F32)
    return (flt * lax.rsqrt(mean + EPS) * gain).astype(BF16)


def silu(gate):
    flt = gate.astype(F32)
    return flt / (1.0 + jnp.exp(-flt))


def mix_kernel(
    pc, qc, kc, count, tp, seqs, length, total_len,
    floats, proj, proj_any, mix, q_gain, k_gain,
    y_recv, lse,
    keys, vals, pool_pad, bias, band, kv_halo, pool_halo, y_buf,
    halo_send, halo_recv, y_send, y_got, y_local,
):
    rows = length // tp
    n_kv = kc // HEAD_DIM
    n_q = qc // HEAD_DIM
    groups = mix.shape[0]
    chan = mix.shape[1]
    i = pl.program_id(0)
    sp_me, me = lax.axis_index("sp"), lax.axis_index("tp")
    offset = sp_me * length
    half_widths = [jnp.left_shift(jnp.int32(1), (me * groups + g) % 4) for g in range(groups)]
    c_gate, c_q, c_ag, c_kv = pc, 2 * pc, 2 * pc + qc, 2 * pc + 2 * qc
    half_pad = 64
    after = (sp_me + 1) % count
    before = (sp_me + count - 1) % count
    peers = [(me + d) % tp for d in range(1, tp)]

    def halo_copies(s):
        made = []
        for side, (target, first) in enumerate(((after, True), (before, False))):
            for kind, (buf, width, col, cols) in enumerate(
                ((kv_halo, WINDOW, c_kv, 2 * kc), (pool_halo, REACH, 0, pc))
            ):
                start = length - width if first else 0
                made.append(
                    pltpu.make_async_remote_copy(
                        src_ref=proj_any.at[s, pl.ds(start, width), pl.ds(col, cols)],
                        dst_ref=buf.at[side, s],
                        send_sem=halo_send.at[side, kind, s],
                        recv_sem=halo_recv.at[side, kind, s],
                        device_id={"sp": target},
                        device_id_type=MESH,
                    )
                )
        return made

    def y_copies(s):
        return [
            pltpu.make_async_remote_copy(
                src_ref=y_buf.at[s, peer],
                dst_ref=y_recv.at[me, s],
                send_sem=y_send.at[d, s],
                recv_sem=y_got.at[d, s],
                device_id={"tp": peer},
                device_id_type=MESH,
            )
            for d, peer in enumerate(peers)
        ]

    def y_own(s):
        return pltpu.make_async_copy(y_buf.at[s, me], y_recv.at[me, s], y_local.at[s])

    @pl.when(i == 0)
    def _():
        barrier = pltpu.get_barrier_semaphore()
        for target in (after, before):
            pl.semaphore_signal(barrier, inc=1, device_id={"sp": target}, device_id_type=MESH)
        for peer in peers:
            pl.semaphore_signal(barrier, inc=1, device_id={"tp": peer}, device_id_type=MESH)
        pl.semaphore_wait(barrier, 2 + len(peers))
        for s in range(seqs):
            for copy in halo_copies(s):
                copy.start()
        ii = lax.broadcasted_iota(jnp.int32, (BLK, 3 * WINDOW), 0)
        jj = lax.broadcasted_iota(jnp.int32, (BLK, 3 * WINDOW), 1) - WINDOW
        dist = jnp.abs(ii - jj)
        for h in range(n_q):
            value = -floats[0, h] * dist.astype(F32) - floats[1, h]
            bias[h] = jnp.where(dist <= WINDOW, value, NEG)
        ti = lax.broadcasted_iota(jnp.int32, (BLK, 2 * BLK), 0)
        tj = lax.broadcasted_iota(jnp.int32, (BLK, 2 * BLK), 1) - half_pad
        rel = tj - ti
        for g in range(groups):
            hw = half_widths[g]
            inside = (rel >= -hw) & (rel <= hw - 1)
            band[g] = jnp.where(inside, 1.0, 0.0).astype(BF16)
        edge = jnp.zeros((half_pad - REACH, pc), BF16)
        pool_pad[0 : half_pad - REACH] = edge
        pool_pad[half_pad + length + REACH :] = edge

    def fill(first, size, kv):
        normed = head_norm(kv[:, :kc], k_gain[...])
        pos = lax.broadcasted_iota(jnp.int32, (size, HEAD_DIM), 0) + (offset + first - WINDOW)
        valid = (pos >= 0) & (pos < total_len)
        ones = jnp.where(valid, 1.0, 0.0).astype(BF16)
        for p in range(n_kv):
            k = normed[:, p * HEAD_DIM : (p + 1) * HEAD_DIM]
            v = kv[:, kc + p * HEAD_DIM : kc + (p + 1) * HEAD_DIM] * ones
            keys[p, first : first + size] = jnp.concatenate([k, k], axis=1)
            vals[2 * p, first : first + size] = jnp.concatenate([v, ones], axis=1)
            vals[2 * p + 1, first : first + size] = jnp.concatenate([ones, v], axis=1)

    low = lax.broadcasted_iota(jnp.int32, (BLK, 2 * HEAD_DIM), 1) < HEAD_DIM

    def step(b, carry):
        start = pl.multiple_of(b * BLK, BLK)
        dest = start // rows
        row = pl.multiple_of(start % rows, BLK)
        here = pl.ds(start, BLK)
        gpos = offset + start + lax.broadcasted_iota(jnp.int32, (BLK, chan), 0)
        for g in range(groups):
            hw = half_widths[g]
            cols = slice(g * chan, (g + 1) * chan)
            window = jnp.dot(band[g], pool_pad[pl.ds(start, 2 * BLK), cols], preferred_element_type=F32)
            lo = jnp.maximum(gpos - hw, 0)
            hi = jnp.minimum(gpos + hw - 1, total_len - 1)
            live = (hi - lo + 1).astype(F32)
            pooled = (window / live - proj[0, here, cols].astype(F32)).astype(BF16)
            mixed = jnp.dot(pooled, mix[g], preferred_element_type=F32)
            gate = proj[0, here, c_gate + g * chan : c_gate + (g + 1) * chan]
            y_buf[i, dest, pl.ds(row, BLK), cols] = (mixed * silu(gate)).astype(BF16)
        queries = head_norm(proj[0, here, c_q : c_q + qc], q_gain[...])
        for p in range(n_kv):
            pair = queries[:, p * 128 : (p + 1) * 128]
            zero = jnp.zeros_like(pair)
            stacked = jnp.concatenate([jnp.where(low, pair, zero), jnp.where(low, zero, pair)], axis=0)
            span = pl.ds(start, 3 * WINDOW)
            scores = lax.dot_general(
                stacked, keys[p, span], (((1,), (1,)), ((), ())), preferred_element_type=F32
            )
            w0 = jnp.exp2(scores[:BLK] + bias[2 * p]).astype(BF16)
            w1 = jnp.exp2(scores[BLK:] + bias[2 * p + 1]).astype(BF16)
            o0 = jnp.dot(w0, vals[2 * p, span], preferred_element_type=F32)
            o1 = jnp.dot(w1, vals[2 * p + 1, span], preferred_element_type=F32)
            num = jnp.where(low, o0, o1)
            tot = jnp.where(low, o1, o0) + 1.0
            den = pltpu.roll(tot, HEAD_DIM, 1)
            gate = proj[0, here, c_ag + p * 128 : c_ag + (p + 1) * 128]
            y_buf[i, dest, pl.ds(row, BLK), pc + p * 128 : pc + (p + 1) * 128] = (
                num / den * silu(gate)
            ).astype(BF16)
            tt = jnp.transpose(tot)
            lse[0, 2 * p : 2 * p + 1, here] = floats[2, 2 * p] + jnp.log(tt[HEAD_DIM : HEAD_DIM + 1])
            lse[0, 2 * p + 1 : 2 * p + 2, here] = floats[2, 2 * p + 1] + jnp.log(tt[0:1])
        return carry

    pool_pad[half_pad : half_pad + length] = proj[0, :, :pc]
    fill(WINDOW, length, proj[0, :, c_kv:])
    for copy in halo_copies(i):
        copy.wait()
    first = jnp.where(sp_me > 0, 1.0, 0.0).astype(BF16)
    last = jnp.where(sp_me < count - 1, 1.0, 0.0).astype(BF16)
    pool_pad[half_pad - REACH : half_pad] = pool_halo[0, i] * first
    pool_pad[half_pad + length : half_pad + length + REACH] = pool_halo[1, i] * last
    fill(0, WINDOW, kv_halo[0, i])
    fill(WINDOW + length, WINDOW, kv_halo[1, i])
    lax.fori_loop(0, length // BLK, step, 0)
    for copy in y_copies(i):
        copy.start()
    y_own(i).start()

    @pl.when(i == seqs - 1)
    def _():
        for t in range(seqs):
            for copy in y_copies(t):
                copy.wait()
            y_own(t).wait()


def out_kernel(tp, seqs, pc, y_ref, w_any, out, w_buf, sems):
    i = pl.program_id(0)
    me = lax.axis_index("tp")
    core = me % 2
    sibling = me + 1 - 2 * core
    local = pltpu.make_async_copy(w_any, w_buf.at[0], sems.at[2])
    swap = pltpu.make_async_remote_copy(
        src_ref=w_any, dst_ref=w_buf.at[1], send_sem=sems.at[0], recv_sem=sems.at[1],
        device_id={"tp": sibling}, device_id_type=MESH,
    )

    @pl.when(i == 0)
    def _():
        barrier = pltpu.get_barrier_semaphore()
        pl.semaphore_signal(barrier, inc=1, device_id={"tp": sibling}, device_id_type=MESH)
        local.start()
        pl.semaphore_wait(barrier, 1)
        swap.start()
        local.wait()

    @pl.when(i == seqs)
    def _():
        swap.wait()

    h = i // seqs
    half = out.shape[-1] // 2
    depth = w_buf.shape[1] * w_buf.shape[3]
    pool_rows = jnp.concatenate([y_ref[p, 0, :, :pc] for p in range(tp)], axis=1)
    attn_rows = jnp.concatenate([y_ref[p, 0, :, pc:] for p in range(tp)], axis=1)
    acc = jnp.dot(pool_rows, w_buf[h, :, 0].reshape(depth, half), preferred_element_type=F32)
    acc = acc + jnp.dot(attn_rows, w_buf[h, :, 1].reshape(depth, half), preferred_element_type=F32)
    col = pl.multiple_of(((core + h) % 2) * half, half)
    out[i % seqs, :, pl.ds(col, half)] = acc.astype(BF16)


def proj_kernel(x_ref, gain, *refs):
    weights, out, wide = refs[:-2], refs[-2], refs[-1]
    tile, seqs, model = x_ref.shape
    flt = x_ref[...].reshape(tile * seqs, model).astype(F32)
    mean = jnp.mean(flt * flt, axis=-1, keepdims=True)
    hidden = (flt * lax.rsqrt(mean + EPS) * gain[...]).astype(BF16)
    col = 0
    for w in weights:
        size = w.shape[1]
        res = jnp.dot(hidden, w[...], preferred_element_type=F32)
        for c in range(0, size, 128):
            n = min(128, size - c)
            wide[:, :n] = res[:, c : c + n]
            for s in range(seqs):
                out[s, :, col + c : col + c + n] = wide[pl.ds(s, tile, stride=seqs), :n].astype(BF16)
        col += size


def body(
    inputs, norm_gain, pool_proj, pool_gate_proj, pool_mix, query_proj, key_proj, value_proj,
    attn_gate_proj, query_gain, key_gain, sink_logit, out_pool, out_attn,
):
    length, seqs, model = inputs.shape
    tp = lax.axis_size("tp")
    tp_index = lax.axis_index("tp")
    count = lax.axis_size("sp")
    total_len = length * count
    pc, qc, kc = pool_proj.shape[1], query_proj.shape[1], key_proj.shape[1]
    width = 2 * pc + 2 * qc + 2 * kc
    n_q = qc // HEAD_DIM
    n_kv = kc // HEAD_DIM
    groups = pool_mix.shape[0]
    rows = length // tp

    half = model // 2
    w_half = jnp.stack([out_pool, out_attn])
    w_half = lax.dynamic_slice_in_dim(w_half, (tp_index % 2) * half, half, 2)
    w_half = lax.all_gather(w_half, "sp", axis=0)

    weights = [pool_proj, pool_gate_proj, query_proj, attn_gate_proj, key_proj, value_proj]
    tile = BLK
    proj = pl.pallas_call(
        proj_kernel,
        grid=(length // tile,),
        in_specs=[
            pl.BlockSpec((tile, seqs, model), lambda t: (t, 0, 0)),
            pl.BlockSpec((1, model), lambda t: (0, 0)),
        ] + [pl.BlockSpec(w.shape, lambda t: (0, 0)) for w in weights],
        out_specs=pl.BlockSpec((seqs, tile, width), lambda t: (0, t, 0)),
        out_shape=jax.ShapeDtypeStruct((seqs, length, width), BF16),
        scratch_shapes=[pltpu.VMEM((tile * seqs, 128), F32)],
        name="projections",
    )(inputs, norm_gain[None], *weights)

    head_ids = tp_index * n_q + jnp.arange(n_q, dtype=jnp.int32)
    slopes = 2.0 ** (-8.0 * (head_ids + 1).astype(F32) / HEADS)
    floats = jnp.stack([slopes * LOG2E, sink_logit * LOG2E, sink_logit])
    q_gain = jnp.tile(query_gain * (HEAD_DIM**-0.5 * LOG2E), n_q)[None]
    k_gain = jnp.tile(key_gain, n_kv)[None]

    smem = pl.BlockSpec(memory_space=pltpu.SMEM)
    full = lambda shape: pl.BlockSpec(shape, lambda s: (0,) * len(shape))
    anywhere = pl.BlockSpec(memory_space=pl.ANY)
    per_seq = lambda *shape: pl.BlockSpec((1,) + shape, lambda i: (i,) + (0,) * len(shape))
    dma = lambda *shape: pltpu.SemaphoreType.DMA(shape)
    y_recv, lse = pl.pallas_call(
        functools.partial(mix_kernel, pc, qc, kc, count, tp, seqs, length, total_len),
        grid=(seqs,),
        in_specs=[
            smem, per_seq(length, width), anywhere,
            full(pool_mix.shape), full((1, qc)), full((1, kc)),
        ],
        out_specs=[anywhere, per_seq(n_q, length)],
        out_shape=[
            jax.ShapeDtypeStruct((tp, seqs, rows, pc + qc), BF16),
            jax.ShapeDtypeStruct((seqs, n_q, length), F32),
        ],
        scratch_shapes=[
            pltpu.VMEM((n_kv, length + 2 * WINDOW, 128), BF16),
            pltpu.VMEM((n_q, length + 2 * WINDOW, 128), BF16),
            pltpu.VMEM((length + 128, pc), BF16),
            pltpu.VMEM((n_q, BLK, 3 * WINDOW), F32),
            pltpu.VMEM((groups, BLK, 2 * BLK), BF16),
            pltpu.VMEM((2, seqs, WINDOW, 2 * kc), BF16),
            pltpu.VMEM((2, seqs, REACH, pc), BF16),
            pltpu.VMEM((seqs, tp, rows, pc + qc), BF16),
            dma(2, 2, seqs), dma(2, 2, seqs),
            dma(tp - 1, seqs), dma(tp - 1, seqs), dma(seqs),
        ],
        compiler_params=pltpu.CompilerParams(collective_id=0, has_side_effects=True),
        name="mixers",
    )(floats, proj, proj, pool_mix, q_gain, k_gain)

    mixed = pl.pallas_call(
        functools.partial(out_kernel, tp, seqs, pc),
        grid=(2 * seqs,),
        in_specs=[
            pl.BlockSpec((tp, 1, rows, pc + qc), lambda i: (0, i % seqs, 0, 0)), anywhere,
        ],
        out_specs=full((seqs, rows, model)),
        out_shape=jax.ShapeDtypeStruct((seqs, rows, model), BF16),
        scratch_shapes=[pltpu.VMEM((2,) + w_half.shape, BF16), dma(3)],
        compiler_params=pltpu.CompilerParams(collective_id=1, has_side_effects=True),
        name="outproj",
    )(y_recv, w_half)
    return jnp.transpose(mixed, (1, 0, 2)), jnp.transpose(lse, (2, 0, 1))


def solution(mesh):
    placed = (
        P("sp", None, None), P(), P(None, "tp"), P(None, "tp"), P("tp", None, None),
        P(None, "tp"), P(None, "tp"), P(None, "tp"), P(None, "tp"),
        P(), P(), P("tp"), P("sp", None), P("sp", None),
    )
    return jax.shard_map(
        body,
        mesh=mesh,
        in_specs=placed,
        out_specs=(P(("sp", "tp"), None, None), P("sp", None, "tp")),
        check_vma=False,
    )
```

```python
import functools
import math

import jax
import jax.numpy as jnp
from jax import lax
from jax.experimental import pallas as pl
from jax.experimental.pallas import tpu as pltpu
from jax.sharding import PartitionSpec as P

HEADS = 16
HEAD_DIM = 64
WINDOW = 128
EPS = 1e-06
NEG = -1e30
LOG2E = math.log2(math.e)
REACH = 16
BLK = 128
F32 = jnp.float32
BF16 = jnp.bfloat16
MESH = pl.DeviceIdType.MESH


def head_ones(cols):
    a = lax.broadcasted_iota(jnp.int32, (cols, cols), 0) // HEAD_DIM
    b = lax.broadcasted_iota(jnp.int32, (cols, cols), 1) // HEAD_DIM
    return jnp.where(a == b, 1.0 / HEAD_DIM, 0.0).astype(BF16)


def head_norm(values, gain):
    flt = values.astype(F32)
    mean = jnp.dot((flt * flt).astype(BF16), head_ones(flt.shape[-1]), preferred_element_type=F32)
    return (flt * lax.rsqrt(mean + EPS) * gain).astype(BF16)


def silu(gate):
    flt = gate.astype(F32)
    return flt / (1.0 + jnp.exp(-flt))


def mix_kernel(
    pc, qc, kc, count, tp, seqs, length, total_len,
    floats, proj, proj_any, mix, q_gain, k_gain,
    y_recv, lse,
    keys, vals, pool_pad, bias, band, kv_halo, pool_halo, y_buf,
    halo_send, halo_recv, y_send, y_got, y_local,
):
    rows = length // tp
    n_kv = kc // HEAD_DIM
    n_q = qc // HEAD_DIM
    groups = mix.shape[0]
    chan = mix.shape[1]
    i = pl.program_id(0)
    sp_me, me = lax.axis_index("sp"), lax.axis_index("tp")
    offset = sp_me * length
    half_widths = [jnp.left_shift(jnp.int32(1), (me * groups + g) % 4) for g in range(groups)]
    c_gate, c_q, c_ag, c_kv = pc, 2 * pc, 2 * pc + qc, 2 * pc + 2 * qc
    half_pad = 64
    after = (sp_me + 1) % count
    before = (sp_me + count - 1) % count
    peers = [(me + d) % tp for d in range(1, tp)]

    def halo_copies(s):
        made = []
        for side, (target, first) in enumerate(((after, True), (before, False))):
            for kind, (buf, width, col, cols) in enumerate(
                ((kv_halo, WINDOW, c_kv, 2 * kc), (pool_halo, REACH, 0, pc))
            ):
                start = length - width if first else 0
                made.append(
                    pltpu.make_async_remote_copy(
                        src_ref=proj_any.at[s, pl.ds(start, width), pl.ds(col, cols)],
                        dst_ref=buf.at[side, s],
                        send_sem=halo_send.at[side, kind, s],
                        recv_sem=halo_recv.at[side, kind, s],
                        device_id={"sp": target},
                        device_id_type=MESH,
                    )
                )
        return made

    def y_copies(s):
        return [
            pltpu.make_async_remote_copy(
                src_ref=y_buf.at[s, peer],
                dst_ref=y_recv.at[me, s],
                send_sem=y_send.at[d, s],
                recv_sem=y_got.at[d, s],
                device_id={"tp": peer},
                device_id_type=MESH,
            )
            for d, peer in enumerate(peers)
        ]

    def y_own(s):
        return pltpu.make_async_copy(y_buf.at[s, me], y_recv.at[me, s], y_local.at[s])

    @pl.when(i == 0)
    def _():
        barrier = pltpu.get_barrier_semaphore()
        for target in (after, before):
            pl.semaphore_signal(barrier, inc=1, device_id={"sp": target}, device_id_type=MESH)
        for peer in peers:
            pl.semaphore_signal(barrier, inc=1, device_id={"tp": peer}, device_id_type=MESH)
        pl.semaphore_wait(barrier, 2 + len(peers))
        for s in range(seqs):
            for copy in halo_copies(s):
                copy.start()
        ii = lax.broadcasted_iota(jnp.int32, (BLK, 3 * WINDOW), 0)
        jj = lax.broadcasted_iota(jnp.int32, (BLK, 3 * WINDOW), 1) - WINDOW
        dist = jnp.abs(ii - jj)
        for h in range(n_q):
            value = -floats[0, h] * dist.astype(F32) - floats[1, h]
            bias[h] = jnp.where(dist <= WINDOW, value, NEG)
        ti = lax.broadcasted_iota(jnp.int32, (BLK, 2 * BLK), 0)
        tj = lax.broadcasted_iota(jnp.int32, (BLK, 2 * BLK), 1) - half_pad
        rel = tj - ti
        for g in range(groups):
            hw = half_widths[g]
            inside = (rel >= -hw) & (rel <= hw - 1)
            band[g] = jnp.where(inside, 1.0, 0.0).astype(BF16)
        edge = jnp.zeros((half_pad - REACH, pc), BF16)
        pool_pad[0 : half_pad - REACH] = edge
        pool_pad[half_pad + length + REACH :] = edge

    def fill(first, size, kv):
        normed = head_norm(kv[:, :kc], k_gain[...])
        pos = lax.broadcasted_iota(jnp.int32, (size, HEAD_DIM), 0) + (offset + first - WINDOW)
        valid = (pos >= 0) & (pos < total_len)
        ones = jnp.where(valid, 1.0, 0.0).astype(BF16)
        for p in range(n_kv):
            k = normed[:, p * HEAD_DIM : (p + 1) * HEAD_DIM]
            v = kv[:, kc + p * HEAD_DIM : kc + (p + 1) * HEAD_DIM] * ones
            keys[p, first : first + size] = jnp.concatenate([k, k], axis=1)
            vals[2 * p, first : first + size] = jnp.concatenate([v, ones], axis=1)
            vals[2 * p + 1, first : first + size] = jnp.concatenate([ones, v], axis=1)

    low = lax.broadcasted_iota(jnp.int32, (BLK, 2 * HEAD_DIM), 1) < HEAD_DIM

    def step(b, carry):
        start = pl.multiple_of(b * BLK, BLK)
        dest = start // rows
        row = pl.multiple_of(start % rows, BLK)
        here = pl.ds(start, BLK)
        gpos = offset + start + lax.broadcasted_iota(jnp.int32, (BLK, chan), 0)
        for g in range(groups):
            hw = half_widths[g]
            cols = slice(g * chan, (g + 1) * chan)
            window = jnp.dot(band[g], pool_pad[pl.ds(start, 2 * BLK), cols], preferred_element_type=F32)
            lo = jnp.maximum(gpos - hw, 0)
            hi = jnp.minimum(gpos + hw - 1, total_len - 1)
            live = (hi - lo + 1).astype(F32)
            pooled = (window / live - proj[0, here, cols].astype(F32)).astype(BF16)
            mixed = jnp.dot(pooled, mix[g], preferred_element_type=F32)
            gate = proj[0, here, c_gate + g * chan : c_gate + (g + 1) * chan]
            y_buf[i, dest, pl.ds(row, BLK), cols] = (mixed * silu(gate)).astype(BF16)
        queries = head_norm(proj[0, here, c_q : c_q + qc], q_gain[...])
        for p in range(n_kv):
            pair = queries[:, p * 128 : (p + 1) * 128]
            zero = jnp.zeros_like(pair)
            stacked = jnp.concatenate([jnp.where(low, pair, zero), jnp.where(low, zero, pair)], axis=0)
            span = pl.ds(start, 3 * WINDOW)
            scores = lax.dot_general(
                stacked, keys[p, span], (((1,), (1,)), ((), ())), preferred_element_type=F32
            )
            w0 = jnp.exp2(scores[:BLK] + bias[2 * p]).astype(BF16)
            w1 = jnp.exp2(scores[BLK:] + bias[2 * p + 1]).astype(BF16)
            o0 = jnp.dot(w0, vals[2 * p, span], preferred_element_type=F32)
            o1 = jnp.dot(w1, vals[2 * p + 1, span], preferred_element_type=F32)
            num = jnp.where(low, o0, o1)
            tot = jnp.where(low, o1, o0) + 1.0
            den = pltpu.roll(tot, HEAD_DIM, 1)
            gate = proj[0, here, c_ag + p * 128 : c_ag + (p + 1) * 128]
            y_buf[i, dest, pl.ds(row, BLK), pc + p * 128 : pc + (p + 1) * 128] = (
                num / den * silu(gate)
            ).astype(BF16)
            tt = jnp.transpose(tot)
            lse[0, 2 * p : 2 * p + 1, here] = floats[2, 2 * p] + jnp.log(tt[HEAD_DIM : HEAD_DIM + 1])
            lse[0, 2 * p + 1 : 2 * p + 2, here] = floats[2, 2 * p + 1] + jnp.log(tt[0:1])
        return carry

    pool_pad[half_pad : half_pad + length] = proj[0, :, :pc]
    fill(WINDOW, length, proj[0, :, c_kv:])
    for copy in halo_copies(i):
        copy.wait()
    first = jnp.where(sp_me > 0, 1.0, 0.0).astype(BF16)
    last = jnp.where(sp_me < count - 1, 1.0, 0.0).astype(BF16)
    pool_pad[half_pad - REACH : half_pad] = pool_halo[0, i] * first
    pool_pad[half_pad + length : half_pad + length + REACH] = pool_halo[1, i] * last
    fill(0, WINDOW, kv_halo[0, i])
    fill(WINDOW + length, WINDOW, kv_halo[1, i])
    per = rows // BLK
    for dest, copy in zip(peers + [me], y_copies(i) + [y_own(i)]):
        lax.fori_loop(0, per, lambda b, c, dest=dest: step(dest * per + b, c), 0)
        copy.start()

    @pl.when(i == seqs - 1)
    def _():
        for t in range(seqs):
            for copy in y_copies(t):
                copy.wait()
            y_own(t).wait()


def out_kernel(tp, seqs, pc, y_ref, w_any, out, w_buf, sems):
    i = pl.program_id(0)
    me = lax.axis_index("tp")
    core = me % 2
    sibling = me + 1 - 2 * core
    local = pltpu.make_async_copy(w_any, w_buf.at[0], sems.at[2])
    swap = pltpu.make_async_remote_copy(
        src_ref=w_any, dst_ref=w_buf.at[1], send_sem=sems.at[0], recv_sem=sems.at[1],
        device_id={"tp": sibling}, device_id_type=MESH,
    )

    @pl.when(i == 0)
    def _():
        barrier = pltpu.get_barrier_semaphore()
        pl.semaphore_signal(barrier, inc=1, device_id={"tp": sibling}, device_id_type=MESH)
        local.start()
        pl.semaphore_wait(barrier, 1)
        swap.start()
        local.wait()

    @pl.when(i == seqs)
    def _():
        swap.wait()

    h = i // seqs
    half = out.shape[-1] // 2
    depth = w_buf.shape[1] * w_buf.shape[3]
    pool_rows = jnp.concatenate([y_ref[p, 0, :, :pc] for p in range(tp)], axis=1)
    attn_rows = jnp.concatenate([y_ref[p, 0, :, pc:] for p in range(tp)], axis=1)
    acc = jnp.dot(pool_rows, w_buf[h, :, 0].reshape(depth, half), preferred_element_type=F32)
    acc = acc + jnp.dot(attn_rows, w_buf[h, :, 1].reshape(depth, half), preferred_element_type=F32)
    col = pl.multiple_of(((core + h) % 2) * half, half)
    out[i % seqs, :, pl.ds(col, half)] = acc.astype(BF16)


def proj_kernel(x_ref, gain, *refs):
    weights, out, wide = refs[:-2], refs[-2], refs[-1]
    tile, seqs, model = x_ref.shape
    flt = x_ref[...].reshape(tile * seqs, model).astype(F32)
    mean = jnp.mean(flt * flt, axis=-1, keepdims=True)
    hidden = (flt * lax.rsqrt(mean + EPS) * gain[...]).astype(BF16)
    col = 0
    for w in weights:
        size = w.shape[1]
        res = jnp.dot(hidden, w[...], preferred_element_type=F32)
        for c in range(0, size, 128):
            n = min(128, size - c)
            wide[:, :n] = res[:, c : c + n]
            for s in range(seqs):
                out[s, :, col + c : col + c + n] = wide[pl.ds(s, tile, stride=seqs), :n].astype(BF16)
        col += size


def body(
    inputs, norm_gain, pool_proj, pool_gate_proj, pool_mix, query_proj, key_proj, value_proj,
    attn_gate_proj, query_gain, key_gain, sink_logit, out_pool, out_attn,
):
    length, seqs, model = inputs.shape
    tp = lax.axis_size("tp")
    tp_index = lax.axis_index("tp")
    count = lax.axis_size("sp")
    total_len = length * count
    pc, qc, kc = pool_proj.shape[1], query_proj.shape[1], key_proj.shape[1]
    width = 2 * pc + 2 * qc + 2 * kc
    n_q = qc // HEAD_DIM
    n_kv = kc // HEAD_DIM
    groups = pool_mix.shape[0]
    rows = length // tp

    half = model // 2
    w_half = jnp.stack([out_pool, out_attn])
    w_half = lax.dynamic_slice_in_dim(w_half, (tp_index % 2) * half, half, 2)
    w_half = lax.all_gather(w_half, "sp", axis=0)

    weights = [pool_proj, pool_gate_proj, query_proj, attn_gate_proj, key_proj, value_proj]
    tile = BLK
    proj = pl.pallas_call(
        proj_kernel,
        grid=(length // tile,),
        in_specs=[
            pl.BlockSpec((tile, seqs, model), lambda t: (t, 0, 0)),
            pl.BlockSpec((1, model), lambda t: (0, 0)),
        ] + [pl.BlockSpec(w.shape, lambda t: (0, 0)) for w in weights],
        out_specs=pl.BlockSpec((seqs, tile, width), lambda t: (0, t, 0)),
        out_shape=jax.ShapeDtypeStruct((seqs, length, width), BF16),
        scratch_shapes=[pltpu.VMEM((tile * seqs, 128), F32)],
        name="projections",
    )(inputs, norm_gain[None], *weights)

    head_ids = tp_index * n_q + jnp.arange(n_q, dtype=jnp.int32)
    slopes = 2.0 ** (-8.0 * (head_ids + 1).astype(F32) / HEADS)
    floats = jnp.stack([slopes * LOG2E, sink_logit * LOG2E, sink_logit])
    q_gain = jnp.tile(query_gain * (HEAD_DIM**-0.5 * LOG2E), n_q)[None]
    k_gain = jnp.tile(key_gain, n_kv)[None]

    smem = pl.BlockSpec(memory_space=pltpu.SMEM)
    full = lambda shape: pl.BlockSpec(shape, lambda s: (0,) * len(shape))
    anywhere = pl.BlockSpec(memory_space=pl.ANY)
    per_seq = lambda *shape: pl.BlockSpec((1,) + shape, lambda i: (i,) + (0,) * len(shape))
    dma = lambda *shape: pltpu.SemaphoreType.DMA(shape)
    y_recv, lse = pl.pallas_call(
        functools.partial(mix_kernel, pc, qc, kc, count, tp, seqs, length, total_len),
        grid=(seqs,),
        in_specs=[
            smem, per_seq(length, width), anywhere,
            full(pool_mix.shape), full((1, qc)), full((1, kc)),
        ],
        out_specs=[anywhere, per_seq(n_q, length)],
        out_shape=[
            jax.ShapeDtypeStruct((tp, seqs, rows, pc + qc), BF16),
            jax.ShapeDtypeStruct((seqs, n_q, length), F32),
        ],
        scratch_shapes=[
            pltpu.VMEM((n_kv, length + 2 * WINDOW, 128), BF16),
            pltpu.VMEM((n_q, length + 2 * WINDOW, 128), BF16),
            pltpu.VMEM((length + 128, pc), BF16),
            pltpu.VMEM((n_q, BLK, 3 * WINDOW), F32),
            pltpu.VMEM((groups, BLK, 2 * BLK), BF16),
            pltpu.VMEM((2, seqs, WINDOW, 2 * kc), BF16),
            pltpu.VMEM((2, seqs, REACH, pc), BF16),
            pltpu.VMEM((seqs, tp, rows, pc + qc), BF16),
            dma(2, 2, seqs), dma(2, 2, seqs),
            dma(tp - 1, seqs), dma(tp - 1, seqs), dma(seqs),
        ],
        compiler_params=pltpu.CompilerParams(collective_id=0, has_side_effects=True),
        name="mixers",
    )(floats, proj, proj, pool_mix, q_gain, k_gain)

    mixed = pl.pallas_call(
        functools.partial(out_kernel, tp, seqs, pc),
        grid=(2 * seqs,),
        in_specs=[
            pl.BlockSpec((tp, 1, rows, pc + qc), lambda i: (0, i % seqs, 0, 0)), anywhere,
        ],
        out_specs=full((seqs, rows, model)),
        out_shape=jax.ShapeDtypeStruct((seqs, rows, model), BF16),
        scratch_shapes=[pltpu.VMEM((2,) + w_half.shape, BF16), dma(3)],
        compiler_params=pltpu.CompilerParams(collective_id=1, has_side_effects=True),
        name="outproj",
    )(y_recv, w_half)
    return jnp.transpose(mixed, (1, 0, 2)), jnp.transpose(lse, (2, 0, 1))


def solution(mesh):
    placed = (
        P("sp", None, None), P(), P(None, "tp"), P(None, "tp"), P("tp", None, None),
        P(None, "tp"), P(None, "tp"), P(None, "tp"), P(None, "tp"),
        P(), P(), P("tp"), P("sp", None), P("sp", None),
    )
    return jax.shard_map(
        body,
        mesh=mesh,
        in_specs=placed,
        out_specs=(P(("sp", "tp"), None, None), P("sp", None, "tp")),
        check_vma=False,
    )
```
